32 devices in a mesh: grp: 2 (over y), sp: 4 (over z), tp: 4 (over x, core).
Axes of the slice: x: 2, y: 2, z: 4, core: 2. Of those that a mesh axis runs over, the one named last changes fastest.
Arguments:
- tokens: bfloat16 [8, 1024, 2048], P('grp', 'sp'), parts along dimension 0, may hold values from -6 to 6
- norm_gain: bfloat16 [2048], replicated, may hold values from 0.099609375 to 1.8984375
- key_weight: bfloat16 [2048, 2048], P(None, 'tp'), may hold values from -0.125 to 0.125
- value_weight: bfloat16 [2048, 2048], P(None, 'tp'), may hold values from -0.125 to 0.125
- break_bias: bfloat16 [8, 1024, 16], P('grp', 'sp', 'tp'), parts along dimension 0, may hold values from -12 to 0
- new_query: bfloat16 [8, 2048], P('grp', 'tp'), parts along dimension 0, may hold values from -6 to 6
Outputs:
- cache_pair: bfloat16 [8, 4, 256, 2, 2048], P(('grp', 'sp'), None, None, None, 'tp'), parts along dimension 0
- cache_bias: bfloat16 [8, 4, 256, 16], P(('grp', 'sp'), None, None, 'tp'), parts along dimension 0
- attended: float32 [8, 2048], P('grp', 'tp'), parts along dimension 0
The draws below stay inside these ranges and needn't reach their ends.
There are 2 independent parts, one for each index of `grp`. The reference program is written for one: setup_inputs(seed, part) draws one part's arguments, and reference() takes and returns one part's arrays. A program takes and returns all parts, laid end to end along the dimension named above; an argument that names none is the same for every part. Nothing has to cross between parts.
All inputs are finite; a program needn't handle non-finite values.
Results may differ from the reference program's by a relative error of at most 0.0064.
Values may be sent and summed in bfloat16 or wider, within the bound.
A program may use at most 64 MiB of HBM per device.

```python
import jax
import jax.numpy as jnp
from jax import lax

D = 2048
HEADS = 16
DH = 128
SEQS = 4
PROMPT_LENGTH = 1024
SPAN = 1
PIECE = 256
N_SP = 4


def draw_break_bias(key, part):
    key_sequence = jax.random.split(key, 6)
    complete_shape = (SEQS, PROMPT_LENGTH, HEADS)
    kind_draw = jax.random.uniform(key_sequence[0], (SEQS, 1, HEADS))
    fast_share = 0.5
    slow_rate = jnp.exp(jax.random.uniform(key_sequence[1], (SEQS, 1, HEADS), minval=jnp.log(0.3), maxval=jnp.log(0.8))) / PROMPT_LENGTH
    fast_rate = jnp.exp(jax.random.uniform(key_sequence[2], (SEQS, 1, HEADS), minval=jnp.log(0.01), maxval=jnp.log(1.0 / 30.0)))
    decay_rate = jnp.where(kind_draw < fast_share, fast_rate, slow_rate)
    block_multiplier = jax.random.uniform(key_sequence[3], (SEQS, 32, 1, HEADS), minval=-0.7, maxval=0.7)
    block_multiplier = jnp.broadcast_to(block_multiplier, (SEQS, 32, PROMPT_LENGTH // 32, HEADS)).reshape(complete_shape)
    constant_level = jnp.log(decay_rate) + block_multiplier
    spike_marker = jax.random.uniform(key_sequence[4], complete_shape) < 4.0 / PROMPT_LENGTH
    spike_threshold = jax.random.uniform(key_sequence[5], complete_shape, minval=-1.4, maxval=0.0)
    return jnp.where(spike_marker, spike_threshold, constant_level).astype(jnp.bfloat16)


def level_of(rng, shape, shards, least, top_value):
    loudness = 1.0
    for axis_at, parts in shards:
        draws = jax.random.uniform(jax.random.fold_in(jax.random.fold_in(rng, 6), axis_at), (parts,), jnp.float32, least / len(shards), top_value / len(shards))
        loudness = loudness * jnp.repeat(jnp.exp(draws), shape[axis_at] // parts).reshape((-1,) + (1,) * (len(shape) - 1 - axis_at))
    return loudness


def centred(rng, shape, scale, most, cuts=(), dtype=jnp.bfloat16):
    array = scale * jax.random.normal(rng, shape, jnp.float32)
    if cuts:
        array = array * level_of(rng, shape, cuts, -0.22, 0.18)
    return jnp.clip(array, -most, most).astype(dtype)


def setup_inputs(seed: int = 0, part: int = 0) -> dict:
    keys = jax.random.split(jax.random.key(seed), 7)
    own_keys = jax.random.split(jax.random.fold_in(keys[6], part), 7)
    return {
        "tokens": centred(own_keys[0], (SEQS, PROMPT_LENGTH, D), 1.0, 6.0, ((1, 4),)),
        "norm_gain": jnp.clip(1.0 + 0.18 * jax.random.normal(keys[1], (D,), jnp.float32), 0.099609375, 1.8984375).astype(jnp.bfloat16),
        "key_weight": centred(keys[2], (D, HEADS * DH), D ** -0.5, 0.125, ((1, 4),)),
        "value_weight": centred(keys[3], (D, HEADS * DH), D ** -0.5, 0.125, ((1, 4),)),
        "break_bias": draw_break_bias(jax.random.fold_in(jax.random.fold_in(keys[6], part), 71), part),
        "new_query": centred(own_keys[5], (SEQS, HEADS * DH), 1.0, 6.0, ((1, 4),)),
    }


norm_eps = 1e-06

def arrange(rows, width):
    shaped = rows.reshape(SEQS, N_SP, SPAN, PIECE, width)
    shaped = jnp.transpose(shaped, (0, 2, 1, 3, 4))
    return shaped.reshape(SEQS * SPAN, N_SP, PIECE, width)

def reference(tokens, norm_gain, key_weight, value_weight, break_bias, new_query):
    widened = tokens.astype(jnp.float32)
    inverse = lax.rsqrt(lax.optimization_barrier(jnp.mean(widened * widened, axis=-1, keepdims=True)) + norm_eps)
    normed = (widened * inverse * norm_gain.astype(jnp.float32)).astype(jnp.bfloat16)
    flat_rows = normed.reshape(SEQS * PROMPT_LENGTH, D)
    key_rows = jnp.dot(flat_rows, key_weight, preferred_element_type=jnp.float32).astype(jnp.bfloat16)
    value_rows = jnp.dot(flat_rows, value_weight, preferred_element_type=jnp.float32).astype(jnp.bfloat16)
    key_rows = key_rows.reshape(SEQS, PROMPT_LENGTH, HEADS * DH)
    value_rows = value_rows.reshape(SEQS, PROMPT_LENGTH, HEADS * DH)
    cache_pair = jnp.stack((arrange(key_rows, HEADS * DH), arrange(value_rows, HEADS * DH)), axis=3)
    cache_bias = arrange(break_bias, HEADS)
    queries = new_query.reshape(SEQS, HEADS, DH).astype(jnp.float32)
    key_heads = key_rows.reshape(SEQS, PROMPT_LENGTH, HEADS, DH).astype(jnp.float32)
    value_heads = value_rows.reshape(SEQS, PROMPT_LENGTH, HEADS, DH).astype(jnp.float32)
    logits = jnp.einsum('shd,sphd->sph', queries, key_heads)
    logits = logits * DH ** (-0.5) + break_bias.astype(jnp.float32)
    keep_log = jax.nn.log_sigmoid(-logits)
    later_sum = lax.cumsum(keep_log, axis=1, reverse=True) - keep_log
    stick_weights = jnp.exp(jax.nn.log_sigmoid(logits) + later_sum).astype(jnp.bfloat16)
    attended = jnp.einsum('sph,sphd->shd', stick_weights.astype(jnp.float32), value_heads)
    return (cache_pair, cache_bias, attended.reshape(SEQS, HEADS * DH))
```

```python
import functools

import jax
import jax.numpy as jnp
from jax import lax
from jax.experimental import pallas as pl
from jax.experimental.pallas import tpu as pltpu
from jax.sharding import PartitionSpec as P

norm_eps = 1e-06


def normalize(tokens, norm_gain):
    widened = tokens.astype(jnp.float32)
    inverse = lax.rsqrt(jnp.mean(widened * widened, axis=-1, keepdims=True) + norm_eps)
    return (widened * inverse * norm_gain.astype(jnp.float32)).astype(jnp.bfloat16)


def project(flat_rows, key_weight, value_weight):
    key_rows = jnp.dot(flat_rows, key_weight, preferred_element_type=jnp.float32).astype(
        jnp.bfloat16
    )
    value_rows = jnp.dot(flat_rows, value_weight, preferred_element_type=jnp.float32).astype(
        jnp.bfloat16
    )
    return (key_rows, value_rows)


def read_placed(new_query, key_rows, value_rows, bias_rows, seq_count):
    block_count, piece, heads_here = bias_rows.shape
    columns = key_rows.shape[2]
    head_size = columns // heads_here
    span = block_count // seq_count
    own_index = lax.axis_index("sp")
    own_seq = own_index // span
    own_part = own_index % span
    own_query = lax.dynamic_slice_in_dim(new_query, own_seq, 1, 0).reshape(heads_here, head_size)
    key_heads = key_rows.reshape(block_count, piece, heads_here, head_size)
    logits = jnp.einsum("hd,nphd->nph", own_query, key_heads, preferred_element_type=jnp.float32)
    logits = logits * head_size ** (-0.5) + bias_rows.astype(jnp.float32)
    keep_log = jax.nn.log_sigmoid(-logits)
    block_totals = jnp.sum(keep_log, axis=1)
    own_slot = (jnp.arange(block_count, dtype=jnp.int32) == own_index)[:, None, None]
    placed = jnp.where(own_slot, block_totals[None], 0.0)
    gathered = lax.psum(placed, "sp")
    same_prompt = lax.dynamic_slice_in_dim(gathered, own_seq * span, span, 0)
    ordered = jnp.transpose(same_prompt, (1, 0, 2)).reshape(block_count * span, heads_here)
    beyond = lax.cumsum(ordered, axis=0, reverse=True) - ordered
    beyond = beyond.reshape(block_count, span, heads_here)
    carried = lax.dynamic_slice_in_dim(beyond, own_part, 1, 1)[:, 0, :]
    later_sum = lax.cumsum(keep_log, axis=1, reverse=True) - keep_log + carried[:, None, :]
    stick_weights = jnp.exp(jax.nn.log_sigmoid(logits) + later_sum).astype(jnp.bfloat16)
    value_heads = value_rows.reshape(block_count, piece, heads_here, head_size)
    mixed = jnp.einsum(
        "nph,nphd->hd", stick_weights, value_heads, preferred_element_type=jnp.float32
    )
    chosen = (jnp.arange(seq_count, dtype=jnp.int32) == own_seq)[:, None]
    partial_rows = jnp.where(chosen, mixed.reshape(1, columns), 0.0)
    return lax.psum(partial_rows, "sp")


def local(tokens, norm_gain, key_weight, value_weight, break_bias, new_query):
    seq_count, tok_rows, width = tokens.shape
    heads_here = break_bias.shape[2]
    block_count = lax.axis_size("sp")
    piece = tok_rows * seq_count // block_count
    columns = key_weight.shape[1]
    normed = normalize(tokens, norm_gain)
    bias_pieces = break_bias.reshape(block_count, piece, heads_here)
    key_rows, value_rows = project(normed.reshape(-1, width), key_weight, value_weight)
    stacked_rows = jnp.stack((key_rows, value_rows), axis=1).reshape(block_count, piece, 2, columns)
    paired, bias_arrived = (
        lax.all_to_all(stacked_rows, "sp", split_axis=0, concat_axis=0, tiled=True),
        lax.all_to_all(bias_pieces, "sp", split_axis=0, concat_axis=0, tiled=True),
    )
    key_rows = paired[:, :, 0]
    value_rows = paired[:, :, 1]
    attended = read_placed(new_query, key_rows, value_rows, bias_arrived, seq_count)
    return (paired[None], bias_arrived[None], attended)


MESH = pl.DeviceIdType.MESH
CHUNKS = 4


def partner_table(n):
    return [sorted((k for k in range(n) if k != c), key=lambda k: (abs(k - c), k)) for c in range(n)]


def pick(table, step, me):
    chosen = jnp.int32(table[0][step])
    for c in range(1, len(table)):
        chosen = jnp.where(me == c, jnp.int32(table[c][step]), chosen)
    return chosen


def gather_kernel(
    n,
    tok_ref,
    gain_ref,
    wk_ref,
    wv_ref,
    bias_ref,
    query_ref,
    pair_ref,
    bias_out,
    att_out,
    tok,
    nrm,
    wk,
    wv,
    keys,
    vals,
    lsc,
    wsc,
    attbuf,
    z_send,
    z_recv,
    x_send,
    x_recv,
    d_send,
    d_recv,
    e_send,
    e_recv,
    b_send,
    b_recv,
    a_send,
    a_recv,
    own_sem,
    w_sem,
):
    me = lax.axis_index("sp")
    t = lax.axis_index("tp")
    tp = lax.axis_size("tp")
    piece, width = tok.shape[1:]
    columns = wk.shape[1]
    heads = bias_ref.shape[1]
    head_size = columns // heads
    quarter = piece // tp
    rows = quarter // CHUNKS
    mate = t + 1 - 2 * lax.rem(t, 2)
    cross = lax.rem(t + 2, tp)
    table = partner_table(n)
    partners = [pick(table, j, me) for j in range(n - 1)]

    barrier = pltpu.get_barrier_semaphore()
    for p in partners:
        pl.semaphore_signal(barrier, inc=1, device_id={"sp": p}, device_id_type=MESH)
    pl.semaphore_signal(barrier, inc=1, device_id={"tp": mate}, device_id_type=MESH)
    pl.semaphore_signal(barrier, inc=1, device_id={"tp": cross}, device_id_type=MESH)

    own_copy = pltpu.make_async_copy(tok_ref.at[me], tok.at[me], own_sem)
    own_copy.start()
    wk_copy = pltpu.make_async_copy(wk_ref, wk, w_sem.at[0])
    wk_copy.start()
    wv_copy = pltpu.make_async_copy(wv_ref, wv, w_sem.at[1])
    wv_copy.start()
    pl.semaphore_wait(barrier, n + 1)

    def span_of(owner, q):
        return pl.ds(pl.multiple_of(owner * quarter + q * rows, rows), rows)

    def hop(src, dst, send, recv, where):
        return pltpu.make_async_remote_copy(
            src_ref=src, dst_ref=dst, send_sem=send, recv_sem=recv, device_id=where, device_id_type=MESH
        )

    def z_copy(p, source, q):
        at = span_of(t, q)
        return hop(
            tok_ref.at[p, at], tok.at[source, at], z_send.at[p, q], z_recv.at[source, q], {"sp": p}
        )

    def share(block, owner, q, send, recv, to):
        at = span_of(owner, q)
        return hop(
            tok.at[block, at], tok.at[block, at], send.at[block, q], recv.at[block, q], {"tp": to}
        )

    def bias_copy(p, source):
        return hop(bias_ref.at[p], bias_out.at[source], b_send.at[p], b_recv.at[source], {"sp": p})

    def att_copy(p, source):
        return hop(attbuf.at[source], attbuf.at[source], a_send.at[p], a_recv.at[source], {"sp": p})

    for p in partners:
        for q in range(CHUNKS):
            z_copy(p, me, q).start()
    for p in partners:
        bias_copy(p, me).start()
    bias_out[me] = bias_ref[me]

    row_at = lax.broadcasted_iota(jnp.int32, (8, columns), 0)
    head_at = lax.broadcasted_iota(jnp.int32, (8, columns), 1) // head_size
    seq_at = lax.broadcasted_iota(jnp.int32, query_ref.shape, 0)
    own_query = jnp.sum(
        jnp.where(seq_at == me, query_ref[...].astype(jnp.float32), 0.0), axis=0, keepdims=True
    )
    spread = jnp.where(row_at == head_at, own_query, 0.0).astype(jnp.bfloat16)
    gain = gain_ref[...].astype(jnp.float32)
    groups = piece // 128
    tile = 128
    out_row = lax.broadcasted_iota(jnp.int32, (2 * tile, 2 * tile), 0)
    in_row = lax.broadcasted_iota(jnp.int32, (2 * tile, 2 * tile), 1)
    zip_rows = jnp.where(in_row == out_row // 2 + lax.rem(out_row, 2) * tile, 1.0, 0.0).astype(
        jnp.bfloat16
    )

    def key_part(block):
        step_rows = 16

        def norm_rows(i, carry):
            at = pl.ds(pl.multiple_of(i * step_rows, step_rows), step_rows)
            widened = tok[block, at, :].astype(jnp.float32)
            inverse = lax.rsqrt(jnp.mean(widened * widened, axis=-1, keepdims=True) + norm_eps)
            nrm[at, :] = (widened * inverse * gain).astype(jnp.bfloat16)
            return carry

        lax.fori_loop(0, piece // step_rows, norm_rows, 0, unroll=2)
        key_rows = jnp.dot(nrm[...], wk[...], preferred_element_type=jnp.float32).astype(jnp.bfloat16)
        keys[...] = key_rows
        logits = lax.dot_general(
            spread, key_rows, (((1,), (1,)), ((), ())), preferred_element_type=jnp.float32
        ) * head_size ** (-0.5)
        for g in range(groups):
            lsc[block * groups + g] = logits[:, g * 128 : (g + 1) * 128]

    def value_part(block):
        value_rows = jnp.dot(nrm[...], wv[...], preferred_element_type=jnp.float32).astype(
            jnp.bfloat16
        )
        vals[block] = value_rows
        for i in range(piece // tile):
            both = jnp.concatenate(
                [keys[i * tile : (i + 1) * tile, :], value_rows[i * tile : (i + 1) * tile, :]], axis=0
            )
            zipped = jnp.dot(zip_rows, both, preferred_element_type=jnp.float32).astype(jnp.bfloat16)
            pair_ref[block, i * tile : (i + 1) * tile] = zipped.reshape(tile, 2, columns)

    previous = me
    own_copy.wait()
    for j in range(n - 1):
        block = partners[j]
        for q in range(CHUNKS):
            z_copy(block, block, q).wait_recv()
            share(block, t, q, x_send, x_recv, cross).start()
            share(block, t, q, d_send, d_recv, mate).start()
            if q == 0:
                if j == 0:
                    wk_copy.wait()
                key_part(previous)
            if q == 1:
                if j == 0:
                    wv_copy.wait()
                value_part(previous)
            if q >= 1:
                share(block, cross, q - 1, x_send, x_recv, cross).wait_recv()
                share(block, cross, q - 1, e_send, e_recv, mate).start()
        share(block, cross, CHUNKS - 1, x_send, x_recv, cross).wait_recv()
        share(block, cross, CHUNKS - 1, e_send, e_recv, mate).start()
        for q in range(CHUNKS):
            share(block, mate, q, d_send, d_recv, mate).wait_recv()
            share(block, mate, q, e_send, e_recv, mate).wait_recv()
        previous = block
    key_part(previous)
    value_part(previous)

    for p in partners:
        bias_copy(p, p).wait_recv()
    after = jnp.where(
        lax.broadcasted_iota(jnp.int32, (128, 128), 0) > lax.broadcasted_iota(jnp.int32, (128, 128), 1),
        1.0,
        0.0,
    )
    carried = jnp.zeros((8, 1), jnp.float32)
    for g in range(n * groups - 1, -1, -1):
        lanes = slice((g % groups) * 128, (g % groups + 1) * 128)
        lsc[g, 0:heads] = lsc[g, 0:heads] + bias_out[g // groups, :, lanes].astype(jnp.float32)
        logits = lsc[g]
        soft = jnp.log1p(jnp.exp(-jnp.abs(logits)))
        take_log = jnp.minimum(logits, 0.0) - soft
        keep_log = jnp.minimum(-logits, 0.0) - soft
        later = (
            jnp.dot(
                keep_log, after, precision=lax.Precision.HIGHEST, preferred_element_type=jnp.float32
            )
            + carried
        )
        wsc[:, g * 128 : (g + 1) * 128] = jnp.exp(take_log + later).astype(jnp.bfloat16)
        carried = carried + jnp.sum(keep_log, axis=1, keepdims=True)
    mixed = jnp.dot(
        wsc[...], vals[...].reshape(n * piece, columns), preferred_element_type=jnp.float32
    )
    attbuf[me] = jnp.sum(jnp.where(row_at == head_at, mixed, 0.0), axis=0, keepdims=True)
    for p in partners:
        att_copy(p, me).start()
    for p in partners:
        for q in range(CHUNKS):
            z_copy(p, me, q).wait_send()
            share(p, t, q, x_send, x_recv, cross).wait_send()
            share(p, t, q, d_send, d_recv, mate).wait_send()
            share(p, cross, q, e_send, e_recv, mate).wait_send()
        bias_copy(p, me).wait_send()
    for p in partners:
        att_copy(p, p).wait_recv()
    for s in range(n):
        att_out[s : s + 1, :] = attbuf[s]
    for p in partners:
        att_copy(p, me).wait_send()


def fused(tokens, norm_gain, key_weight, value_weight, break_bias, new_query):
    n, piece, width = tokens.shape
    heads = break_bias.shape[2]
    columns = key_weight.shape[1]
    bias = jnp.transpose(break_bias, (0, 2, 1))
    vmem = pl.BlockSpec(memory_space=pltpu.VMEM)
    anywhere = pl.BlockSpec(memory_space=pl.ANY)
    dma = pltpu.SemaphoreType.DMA
    pair, bias_placed, attended = pl.pallas_call(
        functools.partial(gather_kernel, n),
        out_shape=(
            jax.ShapeDtypeStruct((n, piece, 2, columns), jnp.bfloat16),
            jax.ShapeDtypeStruct((n, heads, piece), jnp.bfloat16),
            jax.ShapeDtypeStruct((n, columns), jnp.float32),
        ),
        in_specs=[anywhere, vmem, anywhere, anywhere, vmem, vmem],
        out_specs=(vmem, vmem, vmem),
        scratch_shapes=[
            pltpu.VMEM((n, piece, width), jnp.bfloat16),
            pltpu.VMEM((piece, width), jnp.bfloat16),
            pltpu.VMEM(key_weight.shape, jnp.bfloat16),
            pltpu.VMEM(value_weight.shape, jnp.bfloat16),
            pltpu.VMEM((piece, columns), jnp.bfloat16),
            pltpu.VMEM((n, piece, columns), jnp.bfloat16),
            pltpu.VMEM((n * piece // 128, 8, 128), jnp.float32),
            pltpu.VMEM((8, n * piece), jnp.bfloat16),
            pltpu.VMEM((n, 1, columns), jnp.float32),
        ]
        + [dma((n, CHUNKS))] * 8
        + [dma((n,))] * 4
        + [dma, dma((2,))],
        compiler_params=pltpu.CompilerParams(
            collective_id=0, has_side_effects=True, vmem_limit_bytes=48 * 1024 * 1024
        ),
        name="gather_read",
    )(tokens, norm_gain.reshape(1, width), key_weight, value_weight, bias, new_query)
    return (pair[None], jnp.transpose(bias_placed, (0, 2, 1))[None], attended)


def suits(mesh, tokens, break_bias, key_weight):
    n, tp = mesh.shape["sp"], mesh.shape["tp"]
    seq_count, tok_rows, width = tokens.shape
    heads, columns = break_bias.shape[2], key_weight.shape[1]
    return (
        seq_count == n
        and tp == 4
        and n > 1
        and tok_rows % (tp * CHUNKS * 16) == 0
        and tok_rows % 128 == 0
        and heads <= 8
        and columns % heads == 0
        and (columns // heads) % 128 == 0
        and width % 128 == 0
    )


def solution(mesh):
    def step(tokens, norm_gain, key_weight, value_weight, break_bias, new_query):
        if suits(mesh, tokens, break_bias, key_weight):
            return fused(tokens, norm_gain, key_weight, value_weight, break_bias, new_query)
        return local(tokens, norm_gain, key_weight, value_weight, break_bias, new_query)

    return jax.shard_map(
        step,
        mesh=mesh,
        in_specs=(
            P("grp", "sp", None),
            P(),
            P(None, "tp"),
            P(None, "tp"),
            P("grp", "sp", "tp"),
            P("grp", "tp"),
        ),
        out_specs=(
            P(("grp", "sp"), None, None, None, "tp"),
            P(("grp", "sp"), None, None, "tp"),
            P("grp", "tp"),
        ),
        check_vma=False,
    )
```

```python
import functools

import jax
import jax.numpy as jnp
from jax import lax
from jax.experimental import pallas as pl
from jax.experimental.pallas import tpu as pltpu
from jax.sharding import PartitionSpec as P

norm_eps = 1e-06


def normalize(tokens, norm_gain):
    widened = tokens.astype(jnp.float32)
    inverse = lax.rsqrt(jnp.mean(widened * widened, axis=-1, keepdims=True) + norm_eps)
    return (widened * inverse * norm_gain.astype(jnp.float32)).astype(jnp.bfloat16)


def project(flat_rows, key_weight, value_weight):
    key_rows = jnp.dot(flat_rows, key_weight, preferred_element_type=jnp.float32).astype(
        jnp.bfloat16
    )
    value_rows = jnp.dot(flat_rows, value_weight, preferred_element_type=jnp.float32).astype(
        jnp.bfloat16
    )
    return (key_rows, value_rows)


def read_placed(new_query, key_rows, value_rows, bias_rows, seq_count):
    block_count, piece, heads_here = bias_rows.shape
    columns = key_rows.shape[2]
    head_size = columns // heads_here
    span = block_count // seq_count
    own_index = lax.axis_index("sp")
    own_seq = own_index // span
    own_part = own_index % span
    own_query = lax.dynamic_slice_in_dim(new_query, own_seq, 1, 0).reshape(heads_here, head_size)
    key_heads = key_rows.reshape(block_count, piece, heads_here, head_size)
    logits = jnp.einsum("hd,nphd->nph", own_query, key_heads, preferred_element_type=jnp.float32)
    logits = logits * head_size ** (-0.5) + bias_rows.astype(jnp.float32)
    keep_log = jax.nn.log_sigmoid(-logits)
    block_totals = jnp.sum(keep_log, axis=1)
    own_slot = (jnp.arange(block_count, dtype=jnp.int32) == own_index)[:, None, None]
    placed = jnp.where(own_slot, block_totals[None], 0.0)
    gathered = lax.psum(placed, "sp")
    same_prompt = lax.dynamic_slice_in_dim(gathered, own_seq * span, span, 0)
    ordered = jnp.transpose(same_prompt, (1, 0, 2)).reshape(block_count * span, heads_here)
    beyond = lax.cumsum(ordered, axis=0, reverse=True) - ordered
    beyond = beyond.reshape(block_count, span, heads_here)
    carried = lax.dynamic_slice_in_dim(beyond, own_part, 1, 1)[:, 0, :]
    later_sum = lax.cumsum(keep_log, axis=1, reverse=True) - keep_log + carried[:, None, :]
    stick_weights = jnp.exp(jax.nn.log_sigmoid(logits) + later_sum).astype(jnp.bfloat16)
    value_heads = value_rows.reshape(block_count, piece, heads_here, head_size)
    mixed = jnp.einsum(
        "nph,nphd->hd", stick_weights, value_heads, preferred_element_type=jnp.float32
    )
    chosen = (jnp.arange(seq_count, dtype=jnp.int32) == own_seq)[:, None]
    partial_rows = jnp.where(chosen, mixed.reshape(1, columns), 0.0)
    return lax.psum(partial_rows, "sp")


def local(tokens, norm_gain, key_weight, value_weight, break_bias, new_query):
    seq_count, tok_rows, width = tokens.shape
    heads_here = break_bias.shape[2]
    block_count = lax.axis_size("sp")
    piece = tok_rows * seq_count // block_count
    columns = key_weight.shape[1]
    normed = normalize(tokens, norm_gain)
    bias_pieces = break_bias.reshape(block_count, piece, heads_here)
    key_rows, value_rows = project(normed.reshape(-1, width), key_weight, value_weight)
    stacked_rows = jnp.stack((key_rows, value_rows), axis=1).reshape(block_count, piece, 2, columns)
    paired, bias_arrived = (
        lax.all_to_all(stacked_rows, "sp", split_axis=0, concat_axis=0, tiled=True),
        lax.all_to_all(bias_pieces, "sp", split_axis=0, concat_axis=0, tiled=True),
    )
    key_rows = paired[:, :, 0]
    value_rows = paired[:, :, 1]
    attended = read_placed(new_query, key_rows, value_rows, bias_arrived, seq_count)
    return (paired[None], bias_arrived[None], attended)


MESH = pl.DeviceIdType.MESH
CHUNKS = 4


def partner_table(n):
    return [
        [(p,) for p in sorted(set(range(n)) - {c}, key=lambda p: (abs(p - c) > 1, -abs(p - c), p))]
        for c in range(n)
    ]


def send_table(n):
    def rank(c, p):
        span = abs(p - c)
        return (n - 1 - c if p < c else c) > (c if p < c else n - 1 - c), span > 1, -span, p

    return [
        [
            (p, q)
            for p in sorted(set(range(n)) - {c}, key=lambda p: rank(c, p))
            for q in range(CHUNKS)
        ]
        for c in range(n)
    ]


def pick(table, step, part, me):
    chosen = jnp.int32(table[0][step][part])
    for c in range(1, len(table)):
        chosen = jnp.where(me == c, jnp.int32(table[c][step][part]), chosen)
    return chosen


def gather_kernel(
    n,
    tok_ref,
    gain_ref,
    wk_ref,
    wv_ref,
    bias_ref,
    query_ref,
    pair_ref,
    bias_out,
    att_out,
    tok,
    nrm,
    wk,
    wv,
    keys,
    vals,
    lsc,
    wsc,
    attbuf,
    query,
    gains,
    z_send,
    z_recv,
    x_send,
    x_recv,
    d_send,
    d_recv,
    e_send,
    e_recv,
    b_send,
    b_recv,
    a_send,
    a_recv,
    own_sem,
    w_sem,
    s_sem,
):
    me = lax.axis_index("sp")
    t = lax.axis_index("tp")
    tp = lax.axis_size("tp")
    piece, width = tok.shape[1:]
    columns = wk.shape[1]
    heads = bias_ref.shape[1]
    head_size = columns // heads
    half = piece // (tp // 2)
    rows = half // CHUNKS
    side = t // 2
    core = lax.rem(t, 2)
    other = (tp // 2 - 1) - side
    mate = t + 1 - 2 * lax.rem(t, 2)
    cross = lax.rem(t + 2, tp)
    table = partner_table(n)
    partners = [pick(table, j, 0, me) for j in range(n - 1)]
    order = send_table(n)

    barrier = pltpu.get_barrier_semaphore()
    for p in partners:
        pl.semaphore_signal(barrier, inc=1, device_id={"sp": p}, device_id_type=MESH)
        pl.semaphore_signal(barrier, inc=1, device_id={"sp": p, "tp": mate}, device_id_type=MESH)
    pl.semaphore_signal(barrier, inc=1, device_id={"tp": mate}, device_id_type=MESH)
    pl.semaphore_signal(barrier, inc=1, device_id={"tp": cross}, device_id_type=MESH)

    own_copy = pltpu.make_async_copy(tok_ref.at[me], tok.at[me], own_sem)
    own_copy.start()
    wk_copy = pltpu.make_async_copy(wk_ref, wk, w_sem.at[0])
    wk_copy.start()
    wv_copy = pltpu.make_async_copy(wv_ref, wv, w_sem.at[1])
    wv_copy.start()
    small = [
        pltpu.make_async_copy(bias_ref.at[me], bias_out.at[me], s_sem.at[0]),
        pltpu.make_async_copy(query_ref, query, s_sem.at[1]),
        pltpu.make_async_copy(gain_ref, gains, s_sem.at[2]),
    ]
    for copy in small:
        copy.start()
    pl.semaphore_wait(barrier, 2 * n)

    def span_of(owner, q):
        return pl.ds(pl.multiple_of(owner * half + q * rows, rows), rows)

    def hop(src, dst, send, recv, where):
        return pltpu.make_async_remote_copy(
            src_ref=src, dst_ref=dst, send_sem=send, recv_sem=recv, device_id=where, device_id_type=MESH
        )

    def z_copy(p, source, q):
        at = span_of(side, q)
        return hop(
            tok_ref.at[p, at],
            tok.at[source, at],
            z_send.at[p, q],
            z_recv.at[source, q],
            {"sp": p, "tp": mate},
        )

    def share(block, owner, q, send, recv, to):
        at = span_of(owner, q)
        return hop(
            tok.at[block, at], tok.at[block, at], send.at[block, q], recv.at[block, q], {"tp": to}
        )

    def bias_copy(p, source):
        return hop(bias_ref.at[p], bias_out.at[source], b_send.at[p], b_recv.at[source], {"sp": p})

    def att_copy(p, source):
        return hop(attbuf.at[source], attbuf.at[source], a_send.at[p], a_recv.at[source], {"sp": p})

    for p in partners:
        bias_copy(p, me).start()

    @pl.when(core == 0)
    def send_tokens():
        for k in range((n - 1) * CHUNKS):
            p, q = pick(order, k, 0, me), pick(order, k, 1, me)
            z_copy(p, me, q).start()

    for copy in small:
        copy.wait()

    row_at = lax.broadcasted_iota(jnp.int32, (8, columns), 0)
    head_at = lax.broadcasted_iota(jnp.int32, (8, columns), 1) // head_size
    seq_at = lax.broadcasted_iota(jnp.int32, query.shape, 0)
    own_query = jnp.sum(
        jnp.where(seq_at == me, query[...].astype(jnp.float32), 0.0), axis=0, keepdims=True
    )
    spread = jnp.where(row_at == head_at, own_query, 0.0).astype(jnp.bfloat16)
    gain = gains[...].astype(jnp.float32).reshape(1, width)
    groups = piece // 128
    tile = 128
    out_row = lax.broadcasted_iota(jnp.int32, (2 * tile, 2 * tile), 0)
    in_row = lax.broadcasted_iota(jnp.int32, (2 * tile, 2 * tile), 1)
    zip_rows = jnp.where(in_row == out_row // 2 + lax.rem(out_row, 2) * tile, 1.0, 0.0).astype(
        jnp.bfloat16
    )

    def key_part(block):
        step_rows = 16

        def norm_rows(i, carry):
            at = pl.ds(pl.multiple_of(i * step_rows, step_rows), step_rows)
            widened = tok[block, at, :].astype(jnp.float32)
            inverse = lax.rsqrt(jnp.mean(widened * widened, axis=-1, keepdims=True) + norm_eps)
            nrm[at, :] = (widened * inverse * gain).astype(jnp.bfloat16)
            return carry

        lax.fori_loop(0, piece // step_rows, norm_rows, 0, unroll=2)
        key_rows = jnp.dot(nrm[...], wk[...], preferred_element_type=jnp.float32).astype(jnp.bfloat16)
        keys[...] = key_rows
        logits = lax.dot_general(
            spread, key_rows, (((1,), (1,)), ((), ())), preferred_element_type=jnp.float32
        ) * head_size ** (-0.5)
        for g in range(groups):
            lsc[block * groups + g] = logits[:, g * 128 : (g + 1) * 128]

    def value_part(block):
        value_rows = jnp.dot(nrm[...], wv[...], preferred_element_type=jnp.float32).astype(
            jnp.bfloat16
        )
        vals[block] = value_rows
        for i in range(piece // tile):
            both = jnp.concatenate(
                [keys[i * tile : (i + 1) * tile, :], value_rows[i * tile : (i + 1) * tile, :]], axis=0
            )
            zipped = jnp.dot(zip_rows, both, preferred_element_type=jnp.float32).astype(jnp.bfloat16)
            pair_ref[block, i * tile : (i + 1) * tile] = zipped.reshape(tile, 2, columns)

    previous = me
    own_copy.wait()
    def relay(block, start, stop):
        @pl.when(core == 1)
        def relay_chunks():
            for q in range(start, stop):
                if q < CHUNKS:
                    z_copy(block, block, q).wait_recv()
                    share(block, side, q, x_send, x_recv, cross).start()
                    share(block, side, q, d_send, d_recv, mate).start()
                if q >= 1:
                    share(block, other, q - 1, x_send, x_recv, cross).wait_recv()
                    share(block, other, q - 1, e_send, e_recv, mate).start()

    def arrive(block):
        @pl.when(core == 0)
        def wait_chunks():
            for q in range(CHUNKS):
                share(block, side, q, d_send, d_recv, mate).wait_recv()
                share(block, other, q, e_send, e_recv, mate).wait_recv()

    for j in range(n - 1):
        block = partners[j]
        relay(block, 0, 2)
        if j == 0:
            wk_copy.wait()
        key_part(previous)
        relay(block, 2, 3)
        if j == 0:
            wv_copy.wait()
        value_part(previous)
        relay(block, 3, CHUNKS + 1)
        arrive(block)
        previous = block
    key_part(previous)
    value_part(previous)

    for p in partners:
        bias_copy(p, p).wait_recv()
    after = jnp.where(
        lax.broadcasted_iota(jnp.int32, (128, 128), 0) > lax.broadcasted_iota(jnp.int32, (128, 128), 1),
        1.0,
        0.0,
    )
    carried = jnp.zeros((8, 1), jnp.float32)
    for g in range(n * groups - 1, -1, -1):
        lanes = slice((g % groups) * 128, (g % groups + 1) * 128)
        lsc[g, 0:heads] = lsc[g, 0:heads] + bias_out[g // groups, :, lanes].astype(jnp.float32)
        logits = lsc[g]
        soft = jnp.log1p(jnp.exp(-jnp.abs(logits)))
        take_log = jnp.minimum(logits, 0.0) - soft
        keep_log = jnp.minimum(-logits, 0.0) - soft
        later = (
            jnp.dot(
                keep_log, after, precision=lax.Precision.HIGHEST, preferred_element_type=jnp.float32
            )
            + carried
        )
        wsc[:, g * 128 : (g + 1) * 128] = jnp.exp(take_log + later).astype(jnp.bfloat16)
        carried = carried + jnp.sum(keep_log, axis=1, keepdims=True)
    mixed = jnp.dot(
        wsc[...], vals[...].reshape(n * piece, columns), preferred_element_type=jnp.float32
    )
    attbuf[me] = jnp.sum(jnp.where(row_at == head_at, mixed, 0.0), axis=0, keepdims=True)
    for p in partners:
        att_copy(p, me).start()
    for p in partners:
        bias_copy(p, me).wait_send()

    @pl.when(core == 0)
    def sent_tokens():
        for p in partners:
            for q in range(CHUNKS):
                z_copy(p, me, q).wait_send()

    @pl.when(core == 1)
    def sent_shares():
        for p in partners:
            for q in range(CHUNKS):
                share(p, side, q, x_send, x_recv, cross).wait_send()
                share(p, side, q, d_send, d_recv, mate).wait_send()
                share(p, other, q, e_send, e_recv, mate).wait_send()

    for p in partners:
        att_copy(p, p).wait_recv()
    for s in range(n):
        att_out[s : s + 1, :] = attbuf[s]
    for p in partners:
        att_copy(p, me).wait_send()


def fused(tokens, norm_gain, key_weight, value_weight, break_bias, new_query):
    n, piece, width = tokens.shape
    heads = break_bias.shape[2]
    columns = key_weight.shape[1]
    bias = jnp.transpose(break_bias, (0, 2, 1))
    vmem = pl.BlockSpec(memory_space=pltpu.VMEM)
    hbm = pl.BlockSpec(memory_space=pltpu.HBM)
    dma = pltpu.SemaphoreType.DMA
    pair, bias_placed, attended = pl.pallas_call(
        functools.partial(gather_kernel, n),
        out_shape=(
            jax.ShapeDtypeStruct((n, piece, 2, columns), jnp.bfloat16),
            jax.ShapeDtypeStruct((n, heads, piece), jnp.bfloat16),
            jax.ShapeDtypeStruct((n, columns), jnp.float32),
        ),
        in_specs=[hbm] * 6,
        out_specs=(vmem, vmem, vmem),
        scratch_shapes=[
            pltpu.VMEM((n, piece, width), jnp.bfloat16),
            pltpu.VMEM((piece, width), jnp.bfloat16),
            pltpu.VMEM(key_weight.shape, jnp.bfloat16),
            pltpu.VMEM(value_weight.shape, jnp.bfloat16),
            pltpu.VMEM((piece, columns), jnp.bfloat16),
            pltpu.VMEM((n, piece, columns), jnp.bfloat16),
            pltpu.VMEM((n * piece // 128, 8, 128), jnp.float32),
            pltpu.VMEM((8, n * piece), jnp.bfloat16),
            pltpu.VMEM((n, 1, columns), jnp.float32),
            pltpu.VMEM(new_query.shape, jnp.bfloat16),
            pltpu.VMEM((width,), jnp.bfloat16),
        ]
        + [dma((n, CHUNKS))] * 8
        + [dma((n,))] * 4
        + [dma, dma((2,)), dma((3,))],
        compiler_params=pltpu.CompilerParams(
            collective_id=0, has_side_effects=True, vmem_limit_bytes=48 * 1024 * 1024
        ),
        name="gather_read",
    )(tokens, norm_gain, key_weight, value_weight, bias, new_query)
    return (pair[None], jnp.transpose(bias_placed, (0, 2, 1))[None], attended)


def suits(mesh, tokens, break_bias, key_weight):
    n, tp = mesh.shape["sp"], mesh.shape["tp"]
    seq_count, tok_rows, width = tokens.shape
    heads, columns = break_bias.shape[2], key_weight.shape[1]
    return (
        seq_count == n
        and tp == 4
        and n > 1
        and tok_rows % (tp // 2 * CHUNKS * 16) == 0
        and tok_rows % 128 == 0
        and heads <= 8
        and columns % heads == 0
        and (columns // heads) % 128 == 0
        and width % 128 == 0
    )


def solution(mesh):
    def step(tokens, norm_gain, key_weight, value_weight, break_bias, new_query):
        if suits(mesh, tokens, break_bias, key_weight):
            return fused(tokens, norm_gain, key_weight, value_weight, break_bias, new_query)
        return local(tokens, norm_gain, key_weight, value_weight, break_bias, new_query)

    return jax.shard_map(
        step,
        mesh=mesh,
        in_specs=(
            P("grp", "sp", None),
            P(),
            P(None, "tp"),
            P(None, "tp"),
            P("grp", "sp", "tp"),
            P("grp", "tp"),
        ),
        out_specs=(
            P(("grp", "sp"), None, None, None, "tp"),
            P(("grp", "sp"), None, None, "tp"),
            P("grp", "tp"),
        ),
        check_vma=False,
    )
```

```python
import functools

import jax
import jax.numpy as jnp
from jax import lax
from jax.experimental import pallas as pl
from jax.experimental.pallas import tpu as pltpu
from jax.sharding import PartitionSpec as P

norm_eps = 1e-06


def normalize(tokens, norm_gain):
    widened = tokens.astype(jnp.float32)
    inverse = lax.rsqrt(jnp.mean(widened * widened, axis=-1, keepdims=True) + norm_eps)
    return (widened * inverse * norm_gain.astype(jnp.float32)).astype(jnp.bfloat16)


def project(flat_rows, key_weight, value_weight):
    key_rows = jnp.dot(flat_rows, key_weight, preferred_element_type=jnp.float32).astype(
        jnp.bfloat16
    )
    value_rows = jnp.dot(flat_rows, value_weight, preferred_element_type=jnp.float32).astype(
        jnp.bfloat16
    )
    return (key_rows, value_rows)


def read_placed(new_query, key_rows, value_rows, bias_rows, seq_count):
    block_count, piece, heads_here = bias_rows.shape
    columns = key_rows.shape[2]
    head_size = columns // heads_here
    span = block_count // seq_count
    own_index = lax.axis_index("sp")
    own_seq = own_index // span
    own_part = own_index % span
    own_query = lax.dynamic_slice_in_dim(new_query, own_seq, 1, 0).reshape(heads_here, head_size)
    key_heads = key_rows.reshape(block_count, piece, heads_here, head_size)
    logits = jnp.einsum("hd,nphd->nph", own_query, key_heads, preferred_element_type=jnp.float32)
    logits = logits * head_size ** (-0.5) + bias_rows.astype(jnp.float32)
    keep_log = jax.nn.log_sigmoid(-logits)
    block_totals = jnp.sum(keep_log, axis=1)
    own_slot = (jnp.arange(block_count, dtype=jnp.int32) == own_index)[:, None, None]
    placed = jnp.where(own_slot, block_totals[None], 0.0)
    gathered = lax.psum(placed, "sp")
    same_prompt = lax.dynamic_slice_in_dim(gathered, own_seq * span, span, 0)
    ordered = jnp.transpose(same_prompt, (1, 0, 2)).reshape(block_count * span, heads_here)
    beyond = lax.cumsum(ordered, axis=0, reverse=True) - ordered
    beyond = beyond.reshape(block_count, span, heads_here)
    carried = lax.dynamic_slice_in_dim(beyond, own_part, 1, 1)[:, 0, :]
    later_sum = lax.cumsum(keep_log, axis=1, reverse=True) - keep_log + carried[:, None, :]
    stick_weights = jnp.exp(jax.nn.log_sigmoid(logits) + later_sum).astype(jnp.bfloat16)
    value_heads = value_rows.reshape(block_count, piece, heads_here, head_size)
    mixed = jnp.einsum(
        "nph,nphd->hd", stick_weights, value_heads, preferred_element_type=jnp.float32
    )
    chosen = (jnp.arange(seq_count, dtype=jnp.int32) == own_seq)[:, None]
    partial_rows = jnp.where(chosen, mixed.reshape(1, columns), 0.0)
    return lax.psum(partial_rows, "sp")


def local(tokens, norm_gain, key_weight, value_weight, break_bias, new_query):
    seq_count, tok_rows, width = tokens.shape
    heads_here = break_bias.shape[2]
    block_count = lax.axis_size("sp")
    piece = tok_rows * seq_count // block_count
    columns = key_weight.shape[1]
    normed = normalize(tokens, norm_gain)
    bias_pieces = break_bias.reshape(block_count, piece, heads_here)
    key_rows, value_rows = project(normed.reshape(-1, width), key_weight, value_weight)
    stacked_rows = jnp.stack((key_rows, value_rows), axis=1).reshape(block_count, piece, 2, columns)
    paired, bias_arrived = (
        lax.all_to_all(stacked_rows, "sp", split_axis=0, concat_axis=0, tiled=True),
        lax.all_to_all(bias_pieces, "sp", split_axis=0, concat_axis=0, tiled=True),
    )
    key_rows = paired[:, :, 0]
    value_rows = paired[:, :, 1]
    attended = read_placed(new_query, key_rows, value_rows, bias_arrived, seq_count)
    return (paired[None], bias_arrived[None], attended)


MESH = pl.DeviceIdType.MESH
CHUNKS = 4


def partner_table(n):
    return [
        [(p,) for p in sorted(set(range(n)) - {c}, key=lambda p: (abs(p - c) > 1, -abs(p - c), p))]
        for c in range(n)
    ]


def send_table(n):
    def rank(c, p):
        span = abs(p - c)
        return (n - 1 - c if p < c else c) > (c if p < c else n - 1 - c), span > 1, -span, p

    return [
        [
            (p, q)
            for p in sorted(set(range(n)) - {c}, key=lambda p: rank(c, p))
            for q in range(CHUNKS)
        ]
        for c in range(n)
    ]


def pick(table, step, part, me):
    chosen = jnp.int32(table[0][step][part])
    for c in range(1, len(table)):
        chosen = jnp.where(me == c, jnp.int32(table[c][step][part]), chosen)
    return chosen


def gather_kernel(
    n,
    tok_ref,
    gain_ref,
    wk_ref,
    wv_ref,
    bias_ref,
    query_ref,
    pair_ref,
    bias_out,
    att_out,
    tok,
    nrm,
    wk,
    wv,
    keys,
    vals,
    lsc,
    wsc,
    attbuf,
    query,
    gains,
    z_send,
    z_recv,
    x_send,
    x_recv,
    d_send,
    d_recv,
    e_send,
    e_recv,
    b_send,
    b_recv,
    a_send,
    a_recv,
    own_sem,
    w_sem,
    s_sem,
):
    me = lax.axis_index("sp")
    t = lax.axis_index("tp")
    tp = lax.axis_size("tp")
    piece, width = tok.shape[1:]
    columns = wk.shape[1]
    heads = bias_ref.shape[1]
    head_size = columns // heads
    half = piece // (tp // 2)
    rows = half // CHUNKS
    side = t // 2
    core = lax.rem(t, 2)
    other = (tp // 2 - 1) - side
    mate = t + 1 - 2 * lax.rem(t, 2)
    cross = lax.rem(t + 2, tp)
    table = partner_table(n)
    partners = [pick(table, j, 0, me) for j in range(n - 1)]
    order = send_table(n)

    barrier = pltpu.get_barrier_semaphore()
    for p in partners:
        pl.semaphore_signal(barrier, inc=1, device_id={"sp": p}, device_id_type=MESH)
        pl.semaphore_signal(barrier, inc=1, device_id={"sp": p, "tp": mate}, device_id_type=MESH)
    pl.semaphore_signal(barrier, inc=1, device_id={"tp": mate}, device_id_type=MESH)
    pl.semaphore_signal(barrier, inc=1, device_id={"tp": cross}, device_id_type=MESH)

    own_copy = pltpu.make_async_copy(tok_ref.at[me], tok.at[me], own_sem)
    own_copy.start()
    wk_copy = pltpu.make_async_copy(wk_ref, wk, w_sem.at[0])
    wk_copy.start()
    wv_copy = pltpu.make_async_copy(wv_ref, wv, w_sem.at[1])
    wv_copy.start()
    small = [
        pltpu.make_async_copy(bias_ref.at[me], bias_out.at[me], s_sem.at[0]),
        pltpu.make_async_copy(query_ref, query, s_sem.at[1]),
        pltpu.make_async_copy(gain_ref, gains, s_sem.at[2]),
    ]
    for copy in small:
        copy.start()
    pl.semaphore_wait(barrier, 2 * n)

    def span_of(owner, q):
        return pl.ds(pl.multiple_of(owner * half + q * rows, rows), rows)

    def hop(src, dst, send, recv, where):
        return pltpu.make_async_remote_copy(
            src_ref=src, dst_ref=dst, send_sem=send, recv_sem=recv, device_id=where, device_id_type=MESH
        )

    def z_copy(p, source, q):
        at = span_of(side, q)
        return hop(
            tok_ref.at[p, at],
            tok.at[source, at],
            z_send.at[p, q],
            z_recv.at[source, q],
            {"sp": p, "tp": mate},
        )

    def share(block, owner, q, send, recv, to):
        at = span_of(owner, q)
        return hop(
            tok.at[block, at], tok.at[block, at], send.at[block, q], recv.at[block, q], {"tp": to}
        )

    def bias_copy(p, source):
        return hop(bias_ref.at[p], bias_out.at[source], b_send.at[p], b_recv.at[source], {"sp": p})

    def att_copy(p, source):
        return hop(attbuf.at[source], attbuf.at[source], a_send.at[p], a_recv.at[source], {"sp": p})

    for p in partners:
        bias_copy(p, me).start()

    @pl.when(core == 0)
    def send_tokens():
        for k in range((n - 1) * CHUNKS):
            p, q = pick(order, k, 0, me), pick(order, k, 1, me)
            z_copy(p, me, q).start()

    for copy in small:
        copy.wait()

    row_at = lax.broadcasted_iota(jnp.int32, (8, columns), 0)
    head_at = lax.broadcasted_iota(jnp.int32, (8, columns), 1) // head_size
    seq_at = lax.broadcasted_iota(jnp.int32, query.shape, 0)
    own_query = jnp.sum(
        jnp.where(seq_at == me, query[...].astype(jnp.float32), 0.0), axis=0, keepdims=True
    )
    spread = jnp.where(row_at == head_at, own_query, 0.0).astype(jnp.bfloat16)
    gain = gains[...].astype(jnp.float32).reshape(1, width)
    groups = piece // 128
    tile = 128
    out_row = lax.broadcasted_iota(jnp.int32, (2 * tile, 2 * tile), 0)
    in_row = lax.broadcasted_iota(jnp.int32, (2 * tile, 2 * tile), 1)
    zip_rows = jnp.where(in_row == out_row // 2 + lax.rem(out_row, 2) * tile, 1.0, 0.0).astype(
        jnp.bfloat16
    )

    def key_part(block):
        step_rows = 16

        def norm_rows(i, carry):
            at = pl.ds(pl.multiple_of(i * step_rows, step_rows), step_rows)
            widened = tok[block, at, :].astype(jnp.float32)
            inverse = lax.rsqrt(jnp.mean(widened * widened, axis=-1, keepdims=True) + norm_eps)
            nrm[at, :] = (widened * inverse * gain).astype(jnp.bfloat16)
            return carry

        lax.fori_loop(0, piece // step_rows, norm_rows, 0, unroll=2)
        key_rows = jnp.dot(nrm[...], wk[...], preferred_element_type=jnp.float32).astype(jnp.bfloat16)
        keys[...] = key_rows
        logits = lax.dot_general(
            spread, key_rows, (((1,), (1,)), ((), ())), preferred_element_type=jnp.float32
        ) * head_size ** (-0.5)
        for g in range(groups):
            lsc[block * groups + g] = logits[:, g * 128 : (g + 1) * 128]

    def value_part(block):
        value_rows = jnp.dot(nrm[...], wv[...], preferred_element_type=jnp.float32).astype(
            jnp.bfloat16
        )
        vals[block] = value_rows
        for i in range(piece // tile):
            both = jnp.concatenate(
                [keys[i * tile : (i + 1) * tile, :], value_rows[i * tile : (i + 1) * tile, :]], axis=0
            )
            zipped = jnp.dot(zip_rows, both, preferred_element_type=jnp.float32).astype(jnp.bfloat16)
            pair_ref[block, i * tile : (i + 1) * tile] = zipped.reshape(tile, 2, columns)

    previous = me
    own_copy.wait()
    def relay(block, start, stop):
        @pl.when(core == 1)
        def relay_chunks():
            for q in range(start, stop):
                if q < CHUNKS:
                    z_copy(block, block, q).wait_recv()
                    share(block, side, q, x_send, x_recv, cross).start()
                    share(block, side, q, d_send, d_recv, mate).start()
                if q >= 1:
                    share(block, other, q - 1, x_send, x_recv, cross).wait_recv()
                    share(block, other, q - 1, e_send, e_recv, mate).start()

    def arrive(block):
        @pl.when(core == 0)
        def wait_chunks():
            for q in range(CHUNKS):
                share(block, side, q, d_send, d_recv, mate).wait_recv()
                share(block, other, q, e_send, e_recv, mate).wait_recv()

    for j in range(n - 1):
        block = partners[j]
        relay(block, 0, 1)
        if j == 0:
            wk_copy.wait()
        key_part(previous)
        relay(block, 1, 2)
        if j == 0:
            wv_copy.wait()
        value_part(previous)
        relay(block, 2, CHUNKS + 1)
        arrive(block)
        previous = block
    key_part(previous)
    value_part(previous)

    for p in partners:
        bias_copy(p, p).wait_recv()
    after = jnp.where(
        lax.broadcasted_iota(jnp.int32, (128, 128), 0) > lax.broadcasted_iota(jnp.int32, (128, 128), 1),
        1.0,
        0.0,
    )
    carried = jnp.zeros((8, 1), jnp.float32)
    for g in range(n * groups - 1, -1, -1):
        lanes = slice((g % groups) * 128, (g % groups + 1) * 128)
        lsc[g, 0:heads] = lsc[g, 0:heads] + bias_out[g // groups, :, lanes].astype(jnp.float32)
        logits = lsc[g]
        soft = jnp.log1p(jnp.exp(-jnp.abs(logits)))
        take_log = jnp.minimum(logits, 0.0) - soft
        keep_log = jnp.minimum(-logits, 0.0) - soft
        later = (
            jnp.dot(
                keep_log, after, precision=lax.Precision.HIGHEST, preferred_element_type=jnp.float32
            )
            + carried
        )
        wsc[:, g * 128 : (g + 1) * 128] = jnp.exp(take_log + later).astype(jnp.bfloat16)
        carried = carried + jnp.sum(keep_log, axis=1, keepdims=True)
    mixed = jnp.dot(
        wsc[...], vals[...].reshape(n * piece, columns), preferred_element_type=jnp.float32
    )
    attbuf[me] = jnp.sum(jnp.where(row_at == head_at, mixed, 0.0), axis=0, keepdims=True)
    for p in partners:
        att_copy(p, me).start()
    for p in partners:
        bias_copy(p, me).wait_send()

    @pl.when(core == 0)
    def sent_tokens():
        for p in partners:
            for q in range(CHUNKS):
                z_copy(p, me, q).wait_send()

    @pl.when(core == 1)
    def sent_shares():
        for p in partners:
            for q in range(CHUNKS):
                share(p, side, q, x_send, x_recv, cross).wait_send()
                share(p, side, q, d_send, d_recv, mate).wait_send()
                share(p, other, q, e_send, e_recv, mate).wait_send()

    for p in partners:
        att_copy(p, p).wait_recv()
    for s in range(n):
        att_out[s : s + 1, :] = attbuf[s]
    for p in partners:
        att_copy(p, me).wait_send()


def fused(tokens, norm_gain, key_weight, value_weight, break_bias, new_query):
    n, piece, width = tokens.shape
    heads = break_bias.shape[2]
    columns = key_weight.shape[1]
    bias = jnp.transpose(break_bias, (0, 2, 1))
    vmem = pl.BlockSpec(memory_space=pltpu.VMEM)
    hbm = pl.BlockSpec(memory_space=pltpu.HBM)
    dma = pltpu.SemaphoreType.DMA
    pair, bias_placed, attended = pl.pallas_call(
        functools.partial(gather_kernel, n),
        out_shape=(
            jax.ShapeDtypeStruct((n, piece, 2, columns), jnp.bfloat16),
            jax.ShapeDtypeStruct((n, heads, piece), jnp.bfloat16),
            jax.ShapeDtypeStruct((n, columns), jnp.float32),
        ),
        in_specs=[hbm] * 6,
        out_specs=(vmem, vmem, vmem),
        scratch_shapes=[
            pltpu.VMEM((n, piece, width), jnp.bfloat16),
            pltpu.VMEM((piece, width), jnp.bfloat16),
            pltpu.VMEM(key_weight.shape, jnp.bfloat16),
            pltpu.VMEM(value_weight.shape, jnp.bfloat16),
            pltpu.VMEM((piece, columns), jnp.bfloat16),
            pltpu.VMEM((n, piece, columns), jnp.bfloat16),
            pltpu.VMEM((n * piece // 128, 8, 128), jnp.float32),
            pltpu.VMEM((8, n * piece), jnp.bfloat16),
            pltpu.VMEM((n, 1, columns), jnp.float32),
            pltpu.VMEM(new_query.shape, jnp.bfloat16),
            pltpu.VMEM((width,), jnp.bfloat16),
        ]
        + [dma((n, CHUNKS))] * 8
        + [dma((n,))] * 4
        + [dma, dma((2,)), dma((3,))],
        compiler_params=pltpu.CompilerParams(
            collective_id=0, has_side_effects=True, vmem_limit_bytes=48 * 1024 * 1024
        ),
        name="gather_read",
    )(tokens, norm_gain, key_weight, value_weight, bias, new_query)
    return (pair[None], jnp.transpose(bias_placed, (0, 2, 1))[None], attended)


def suits(mesh, tokens, break_bias, key_weight):
    n, tp = mesh.shape["sp"], mesh.shape["tp"]
    seq_count, tok_rows, width = tokens.shape
    heads, columns = break_bias.shape[2], key_weight.shape[1]
    return (
        seq_count == n
        and tp == 4
        and n > 1
        and tok_rows % (tp // 2 * CHUNKS * 16) == 0
        and tok_rows % 128 == 0
        and heads <= 8
        and columns % heads == 0
        and (columns // heads) % 128 == 0
        and width % 128 == 0
    )


def solution(mesh):
    def step(tokens, norm_gain, key_weight, value_weight, break_bias, new_query):
        if suits(mesh, tokens, break_bias, key_weight):
            return fused(tokens, norm_gain, key_weight, value_weight, break_bias, new_query)
        return local(tokens, norm_gain, key_weight, value_weight, break_bias, new_query)

    return jax.shard_map(
        step,
        mesh=mesh,
        in_specs=(
            P("grp", "sp", None),
            P(),
            P(None, "tp"),
            P(None, "tp"),
            P("grp", "sp", "tp"),
            P("grp", "tp"),
        ),
        out_specs=(
            P(("grp", "sp"), None, None, None, "tp"),
            P(("grp", "sp"), None, None, "tp"),
            P("grp", "tp"),
        ),
        check_vma=False,
    )
```
